32 devices in a mesh: sp: 8 (over z, y), tp: 4 (over x, core).
Axes of the slice: x: 2, y: 2, z: 4, core: 2. Of those that a mesh axis runs over, the one named last changes fastest.
Arguments:
- resid: bfloat16 [2048, 2048], P(('sp', 'tp')), may hold values from -0.21875 to 0.21875
- query_a: bfloat16 [2048, 1024], P('sp', 'tp'), may hold values from -6 to 6
- key_a: bfloat16 [2048, 256], P('sp', 'tp'), may hold values from -6 to 6
- value_a: bfloat16 [2048, 256], P('sp', 'tp'), may hold values from -6 to 6
- query_b: bfloat16 [2048, 1024], P('sp', 'tp'), may hold values from -6 to 6
- key_b: bfloat16 [2048, 512], P('sp', 'tp'), may hold values from -6 to 6
- value_b: bfloat16 [2048, 512], P('sp', 'tp'), may hold values from -6 to 6
- gain_qa: float32 [64], replicated, may hold values from 0.1 to 8
- gain_ka: float32 [64], replicated, may hold values from 0.1 to 8
- gain_qb: float32 [128], replicated, may hold values from 0.1 to 8
- gain_kb: float32 [128], replicated, may hold values from 0.1 to 8
- w_out_a: bfloat16 [1024, 2048], P('tp'), may hold values from -0.125 to 0.125
- w_out_b: bfloat16 [1024, 2048], P('tp'), may hold values from -0.125 to 0.125
- norm_gain: float32 [2048], replicated, may hold values from 0.1 to 1.9
- w_up: bfloat16 [2048, 8192], P('sp', 'tp'), may hold values from -0.125 to 0.125
- w_down: bfloat16 [8192, 2048], P('tp', 'sp'), may hold values from -0.0625 to 0.0625
Outputs:
- result: bfloat16 [2048, 2048], P(('sp', 'tp'))
The draws below stay inside these ranges and needn't reach their ends.
All inputs are finite; a program needn't handle non-finite values.
Results may differ from the reference program's by a relative error of at most 0.02.
The reference program's roundings to bfloat16 on the way count: a program that leaves them out, or rounds other values in their place, can miss the bound.
Values may be sent and summed in bfloat16 or wider, within the bound.
A program may use at most 128 MiB of HBM per device.

```python
import math
import jax
import jax.numpy as jnp
from jax import lax

D = 2048
FF = 8192
HD_A = 64
HD_B = 128
HEADS_A = 16
HEADS_B = 8
KV_A = 4
KV_B = 4
GRID_W = 64
TOKENS = 2048
ATT_W = 2048


def pair_draw(key, heads, kv_heads, width, salt):
    base = jax.random.fold_in(key, salt)
    keys = jnp.clip(jax.random.normal(jax.random.fold_in(base, 1), (TOKENS, kv_heads * width), jnp.float32), -6.0, 6.0)
    queries = jnp.clip(jax.random.normal(jax.random.fold_in(base, 2), (TOKENS, heads * width), jnp.float32), -6.0, 6.0)
    return (queries.astype(jnp.bfloat16), keys.astype(jnp.bfloat16))


def gain_draw(key, width, salt):
    inner = jax.random.fold_in(key, salt)
    return jnp.clip(1.0 + 0.18 * jax.random.normal(inner, (width,), jnp.float32), 0.1, 1.9)


def draw_query_a(key, part):
    return pair_draw(key, HEADS_A, KV_A, HD_A, 101)[0]


def draw_key_a(key, part):
    return pair_draw(key, HEADS_A, KV_A, HD_A, 101)[1]


def draw_query_b(key, part):
    return pair_draw(key, HEADS_B, KV_B, HD_B, 202)[0]


def draw_key_b(key, part):
    return pair_draw(key, HEADS_B, KV_B, HD_B, 202)[1]


def draw_gain_qa(key, part):
    return gain_draw(key, HD_A, 31)


def draw_gain_ka(key, part):
    return gain_draw(key, HD_A, 32)


def draw_gain_qb(key, part):
    return gain_draw(key, HD_B, 33)


def draw_gain_kb(key, part):
    return gain_draw(key, HD_B, 34)


def shard_levels(own_key, extent, pieces, least, high):
    factor_of = 1.0
    for dim, blocks in pieces:
        heights = jax.random.uniform(jax.random.fold_in(jax.random.fold_in(own_key, 6), dim), (blocks,), jnp.float32, least / len(pieces), high / len(pieces))
        factor_of = factor_of * jnp.repeat(jnp.exp(heights), extent[dim] // blocks).reshape((-1,) + (1,) * (len(extent) - 1 - dim))
    return factor_of


def normal_values(rng, extent, scale, reach, cuts=(), kind=jnp.bfloat16):
    entries = jax.random.normal(rng, extent, jnp.float32) * scale
    if len(cuts) > 0:
        entries = shard_levels(rng, extent, cuts, -0.22, 0.18) * entries
    return jnp.clip(entries, min=-reach, max=reach).astype(kind)


def setup_inputs(seed: int = 0) -> dict:
    key_of = jax.random.split(jax.random.key(seed), 17)
    return {
        "resid": normal_values(key_of[0], (TOKENS, D), 0.015, 0.21875, ((0, 32),)),
        "query_a": draw_query_a(jax.random.fold_in(key_of[16], 71), 0),
        "key_a": draw_key_a(jax.random.fold_in(key_of[16], 71), 0),
        "value_a": normal_values(key_of[3], (TOKENS, KV_A * HD_A), 1.0, 6.0, ((0, 8), (1, 4))),
        "query_b": draw_query_b(jax.random.fold_in(key_of[16], 71), 0),
        "key_b": draw_key_b(jax.random.fold_in(key_of[16], 71), 0),
        "value_b": normal_values(key_of[6], (TOKENS, KV_B * HD_B), 1.0, 6.0, ((0, 8), (1, 4))),
        "gain_qa": draw_gain_qa(jax.random.fold_in(key_of[16], 71), 0),
        "gain_ka": draw_gain_ka(jax.random.fold_in(key_of[16], 71), 0),
        "gain_qb": draw_gain_qb(jax.random.fold_in(key_of[16], 71), 0),
        "gain_kb": draw_gain_kb(jax.random.fold_in(key_of[16], 71), 0),
        "w_out_a": normal_values(key_of[11], (HEADS_A * HD_A, D), ATT_W ** -0.5, 0.125, ((0, 4),)),
        "w_out_b": normal_values(key_of[12], (HEADS_B * HD_B, D), ATT_W ** -0.5, 0.125, ((0, 4),)),
        "norm_gain": jnp.clip(1.0 + 0.18 * jax.random.normal(key_of[13], (D,), jnp.float32), 0.1, 1.9),
        "w_up": normal_values(key_of[14], (D, FF), D ** -0.5, 0.125, ((0, 8), (1, 4))),
        "w_down": normal_values(key_of[15], (FF, D), FF ** -0.5, 0.0625, ((0, 4), (1, 8))),
    }


EPS = 1e-06

def tables(count, width):
    pos = jnp.arange(count, dtype=jnp.int32)
    grid_rows = (pos // GRID_W).astype(jnp.float32)
    grid_cols = (pos % GRID_W).astype(jnp.float32)
    quarter = width // 4
    freqs = 10000.0 ** (-(2.0 * jnp.arange(quarter, dtype=jnp.float32)) / (width // 2))
    ang_r = grid_rows[:, None] * freqs
    ang_c = grid_cols[:, None] * freqs
    angles = jnp.concatenate([ang_r, ang_r, ang_c, ang_c], axis=-1)
    return (jnp.cos(angles), jnp.sin(angles))

def norm_rope(values, gain, width):
    count = values.shape[0]
    flat = values.astype(jnp.float32).reshape(count, -1, width)
    flat = flat * lax.rsqrt(lax.optimization_barrier(jnp.mean(flat * flat, axis=-1, keepdims=True)) + EPS) * gain.astype(jnp.float32)
    cosine, sine = tables(count, width)
    one, two, three, four = jnp.split(flat, 4, axis=-1)
    turned = jnp.concatenate([-two, one, -four, three], axis=-1)
    return (flat * cosine[:, None, :] + turned * sine[:, None, :]).astype(jnp.bfloat16)

def attend(queries, keys, values, width):
    count, heads = (queries.shape[0], queries.shape[1])
    kv_heads = keys.shape[1]
    groups = heads // kv_heads
    block = math.gcd(count, 256)
    keys32 = keys.astype(jnp.float32)
    vals32 = values.astype(jnp.float32).reshape(count, kv_heads, width)
    blocks = queries.reshape(count // block, block, kv_heads, groups, width)
    scale = width ** (-0.5)

    def one_block(qblock):
        scores = jnp.einsum('rkgd,pkd->kgrp', qblock.astype(jnp.float32), keys32) * scale
        top = lax.optimization_barrier(jnp.max(scores, axis=-1, keepdims=True))
        expo = jnp.exp(scores - top)
        probs = expo.astype(jnp.bfloat16).astype(jnp.float32)
        summed = jnp.einsum('kgrp,pkd->kgrd', probs, vals32)
        outputs = summed / lax.optimization_barrier(jnp.sum(expo, axis=-1))[..., None]
        return jnp.transpose(outputs, (2, 0, 1, 3)).reshape(block, heads * width).astype(jnp.bfloat16)
    return lax.map(one_block, blocks).reshape(count, heads * width)

def reference(resid, query_a, key_a, value_a, query_b, key_b, value_b, gain_qa, gain_ka, gain_qb, gain_kb, w_out_a, w_out_b, norm_gain, w_up, w_down):
    width_a = gain_qa.shape[0]
    width_b = gain_qb.shape[0]
    attn_a = attend(norm_rope(query_a, gain_qa, width_a), norm_rope(key_a, gain_ka, width_a), value_a, width_a)
    attn_b = attend(norm_rope(query_b, gain_qb, width_b), norm_rope(key_b, gain_kb, width_b), value_b, width_b)
    proj = jnp.dot(attn_a, w_out_a, preferred_element_type=jnp.float32) + jnp.dot(attn_b, w_out_b, preferred_element_type=jnp.float32)
    mid = (resid.astype(jnp.float32) + proj).astype(jnp.bfloat16)
    midf = mid.astype(jnp.float32)
    normed = (midf * lax.rsqrt(lax.optimization_barrier(jnp.mean(midf * midf, axis=-1, keepdims=True)) + EPS) * norm_gain).astype(jnp.bfloat16)
    hidden = jnp.square(jax.nn.relu(jnp.dot(normed, w_up, preferred_element_type=jnp.float32))).astype(jnp.bfloat16)
    return (midf + jnp.dot(hidden, w_down, preferred_element_type=jnp.float32)).astype(jnp.bfloat16)
```

```python
import math

import jax
import jax.numpy as jnp
import numpy as np
from jax import lax
from jax.experimental import pallas as pl
from jax.experimental.pallas import tpu as pltpu
from jax.sharding import PartitionSpec as P

GRID_W = 64


EPS = 1e-06


def norm_rope(values, gain, places):
    width = gain.shape[0]
    count = values.shape[0]
    flat = values.astype(jnp.float32).reshape(count, -1, width)
    flat = flat * lax.rsqrt(jnp.mean(flat * flat, axis=-1, keepdims=True) + EPS) * gain
    grid_rows = (places // GRID_W).astype(jnp.float32)
    grid_cols = (places % GRID_W).astype(jnp.float32)
    quarter = width // 4
    freqs = 10000.0 ** (-(2.0 * jnp.arange(quarter, dtype=jnp.float32)) / (width // 2))
    ang_r = grid_rows[:, None] * freqs
    ang_c = grid_cols[:, None] * freqs
    angles = jnp.concatenate([ang_r, ang_r, ang_c, ang_c], axis=-1)
    one, two, three, four = jnp.split(flat, 4, axis=-1)
    turned = jnp.concatenate([-two, one, -four, three], axis=-1)
    return (flat * jnp.cos(angles)[:, None, :] + turned * jnp.sin(angles)[:, None, :]).astype(
        jnp.bfloat16
    )


def fold_block(state, queries, key_block, value_block, scale):
    running, total, accum = state
    scores = (
        jnp.einsum("rkgd,pkd->kgrp", queries, key_block, preferred_element_type=jnp.float32) * scale
    )
    newest = jnp.maximum(running, jnp.max(scores, axis=-1))
    factor = jnp.exp(running - newest)
    expo = jnp.exp(scores - newest[..., None])
    total = total * factor + jnp.sum(expo, axis=-1)
    accum = accum * factor[..., None] + jnp.einsum(
        "kgrp,pkd->kgrd", expo.astype(jnp.bfloat16), value_block, preferred_element_type=jnp.float32
    )
    return (newest, total, accum)


def sweep_keys(state, queries, key_piece, value_piece, scale):
    length = key_piece.shape[0]
    block = math.gcd(length, 2048)
    blocks = length // block
    if blocks == 1:
        return fold_block(state, queries, key_piece, value_piece, scale)
    key_blocks = key_piece.reshape((blocks, block) + key_piece.shape[1:])
    value_blocks = value_piece.reshape((blocks, block) + value_piece.shape[1:])

    def advance(carry, pair):
        return (fold_block(carry, queries, pair[0], pair[1], scale), None)

    state, unused = lax.scan(advance, state, (key_blocks, value_blocks))
    return state


def start_state(queries):
    shape = (queries.shape[1], queries.shape[2], queries.shape[0])
    return (
        jnp.full(shape, -1e30, jnp.float32),
        jnp.zeros(shape, jnp.float32),
        jnp.zeros(shape + (queries.shape[3],), jnp.float32),
    )


def finish(state):
    running, total, accum = state
    outputs = accum / total[..., None]
    count = outputs.shape[2]
    return jnp.transpose(outputs, (2, 0, 1, 3)).reshape(count, -1).astype(jnp.bfloat16)


def local(
    resid,
    query_a,
    key_a,
    value_a,
    query_b,
    key_b,
    value_b,
    gain_qa,
    gain_ka,
    gain_qb,
    gain_kb,
    w_out_a,
    w_out_b,
    norm_gain,
    w_up,
    w_down,
):
    count = query_a.shape[0]
    width_a = gain_qa.shape[0]
    width_b = gain_qb.shape[0]
    places = lax.axis_index("sp") * count + jnp.arange(count, dtype=jnp.int32)
    keys_a = norm_rope(key_a, gain_ka, places)
    keys_b = norm_rope(key_b, gain_kb, places)
    heads_kv_a = keys_a.shape[1]
    heads_kv_b = keys_b.shape[1]
    queries_a = norm_rope(query_a, gain_qa, places)
    queries_b = norm_rope(query_b, gain_qb, places)
    queries_a = queries_a.reshape(count, heads_kv_a, queries_a.shape[1] // heads_kv_a, width_a)
    queries_b = queries_b.reshape(count, heads_kv_b, queries_b.shape[1] // heads_kv_b, width_b)
    values_a = value_a.reshape(count, heads_kv_a, width_a)
    values_b = value_b.reshape(count, heads_kv_b, width_b)
    state_a = sweep_keys(
        start_state(queries_a),
        queries_a,
        lax.all_gather(keys_a, "sp", axis=0, tiled=True),
        lax.all_gather(values_a, "sp", axis=0, tiled=True),
        width_a ** (-0.5),
    )
    state_b = sweep_keys(
        start_state(queries_b),
        queries_b,
        lax.all_gather(keys_b, "sp", axis=0, tiled=True),
        lax.all_gather(values_b, "sp", axis=0, tiled=True),
        width_b ** (-0.5),
    )
    attn_a = finish(state_a)
    attn_b = finish(state_b)
    rows_a, rows_b = (
        lax.all_to_all(attn_a, "tp", split_axis=0, concat_axis=1, tiled=True),
        lax.all_to_all(attn_b, "tp", split_axis=0, concat_axis=1, tiled=True),
    )
    whole_a, whole_b = (
        lax.all_gather(w_out_a, "tp", axis=0, tiled=True),
        lax.all_gather(w_out_b, "tp", axis=0, tiled=True),
    )
    proj = jnp.dot(rows_a, whole_a, preferred_element_type=jnp.float32) + jnp.dot(
        rows_b, whole_b, preferred_element_type=jnp.float32
    )
    mid = (resid.astype(jnp.float32) + proj).astype(jnp.bfloat16)
    midf = mid.astype(jnp.float32)
    normed = (
        midf * lax.rsqrt(jnp.mean(midf * midf, axis=-1, keepdims=True) + EPS) * norm_gain
    ).astype(jnp.bfloat16)
    up_whole, down_whole = (
        lax.all_gather(w_up, "sp", axis=0, tiled=True),
        lax.all_gather(w_down, "sp", axis=1, tiled=True),
    )
    hidden = jnp.square(
        jax.nn.relu(
            jnp.dot(
                lax.all_gather(normed, "tp", axis=0, tiled=True),
                up_whole,
                preferred_element_type=jnp.float32,
            )
        )
    ).astype(jnp.bfloat16)
    mixed = lax.psum_scatter(
        jnp.dot(hidden, down_whole, preferred_element_type=jnp.float32).astype(jnp.bfloat16),
        "tp",
        scatter_dimension=0,
        tiled=True,
    ).astype(jnp.float32)
    return (midf + mixed).astype(jnp.bfloat16)


MESH = pl.DeviceIdType.MESH
INNER = 2
SIDES = 2
LANES = 128
HALVES = 2
FAR = (3, 1, 2)


def remote(src, dst, send, recv, target):
    return pltpu.make_async_remote_copy(
        src_ref=src,
        dst_ref=dst,
        send_sem=send,
        recv_sem=recv,
        device_id=target,
        device_id_type=MESH,
    )


def flip(place, k):
    bit = 1
    while bit <= k:
        if k & bit:
            place = place + bit - 2 * bit * lax.rem(place // bit, 2)
        bit *= 2
    return place


def far_order(outer):
    return FAR if outer == 4 else tuple(range(outer - 1, 0, -1))


def arrive(dst, sem):
    pltpu.make_async_copy(dst, dst, sem).wait()


class Mail:
    def __init__(self, sems):
        self.sems = sems
        self.sent = []

    def ship(self, src, dst, recv, target, when=None):
        send = self.sems.at[len(self.sent)]
        self.sent.append((src, send, when))

        def start():
            remote(src, dst, send, recv, target).start()

        if when is None:
            start()
        else:
            pl.when(when)(start)

    def close(self):
        for src, send, when in self.sent:

            def finish(src=src, send=send):
                arrive(src, send)

            if when is None:
                finish()
            else:
                pl.when(when)(finish)


def layer_kernel(
    outer,
    scales,
    ka_t,
    va_t,
    k_b,
    v_b,
    q_a,
    q_b,
    row_table,
    col_table,
    gain_qa,
    gain_ka,
    gain_qb,
    gain_kb,
    norm_gain,
    resid_hbm,
    out_a_hbm,
    out_b_hbm,
    up,
    down,
    out,
    resid,
    out_a,
    out_b,
    kv_all,
    attn,
    up_all,
    down_all,
    pc_out,
    pc_in,
    px_out,
    px_in,
    mid,
    tokens,
    hidden,
    core_out,
    core_in,
    side_out,
    side_in,
    chain_out,
    chain_in,
    held,
    total_sum,
    s_all,
    s_here,
    r_kv,
    r_up,
    r_down,
    r_pc,
    r_px,
    r_tok,
    r_core,
    r_side,
    r_chain,
):
    f32 = jnp.float32
    bf16 = jnp.bfloat16
    sp = lax.axis_index("sp")
    tp = lax.axis_index("tp")
    z = sp // INNER
    y = sp % INNER
    x = tp // INNER
    c = tp % INNER
    lanes = SIDES * INNER
    rows = up.shape[0]
    units = up_all.shape[1]
    count = q_a.shape[0]
    total = outer * INNER
    band, width = mid.shape
    slab = down_all.shape[2] // total
    mail = Mail(s_all)
    z_far = [flip(z, k) for k in far_order(outer)]
    at_z = [{"sp": p * INNER + y} for p in z_far]
    at_y = {"sp": z * INNER + 1 - y}
    at_x = {"tp": (1 - x) * INNER + c}
    at_c = {"tp": x * INNER + 1 - c}
    x_lane = (1 - x) * INNER + c
    has_above = z < outer - 1
    has_below = z > 0
    above = {"sp": jnp.minimum(z + 1, outer - 1) * INNER + y}
    below = {"sp": jnp.maximum(z - 1, 0) * INNER + y}

    barrier = pltpu.get_barrier_semaphore()
    for target in at_z + [at_y, at_x, at_c]:
        pl.semaphore_signal(barrier, inc=1, device_id=target, device_id_type=MESH)

    here = []

    def fetch(src, dst):
        copy = pltpu.make_async_copy(src, dst, s_here.at[len(here)])
        copy.start()
        here.append(copy)
        return copy

    def up_piece(target):
        return up.at[:, pl.ds(pl.multiple_of(target * units, units), units)]

    def up_place(source):
        return up_all.at[pl.ds(pl.multiple_of(source * rows, rows), rows), :]

    def down_piece(h, target):
        at = pl.ds(pl.multiple_of(target * units, units), units)
        return down.at[at, h * slab : (h + 1) * slab]

    def down_place(h, source):
        return down_all.at[h, :, pl.ds(pl.multiple_of(source * slab, slab), slab)]

    get_out_a = fetch(out_a_hbm, out_a)
    get_out_b = fetch(out_b_hbm, out_b)
    get_resid = fetch(resid_hbm, resid)
    get_up = fetch(up_piece(z), up_place(sp))
    get_down = [fetch(down_piece(h, z), down_place(h, sp)) for h in range(HALVES)]

    lane = lax.broadcasted_iota(jnp.int32, (count, LANES), 1)
    low = lane < LANES // 2
    grid_rows = count // GRID_W
    col_part = col_table[...]
    table = jnp.concatenate(
        [col_part + row_table[pl.ds(sp * grid_rows + r, 1), :] for r in range(grid_rows)], axis=0
    )
    cos_a, sin_a, cos_b, sin_b = [table[:, n * LANES : (n + 1) * LANES] for n in range(4)]

    def spin(value, quarter):
        even = lax.rem(lane // quarter, 2) == 0
        ahead = pltpu.roll(value, LANES - quarter, 1)
        behind = pltpu.roll(value, quarter, 1)
        return jnp.where(even, -ahead, behind)

    def turn_b(raw, gain):
        value = raw.astype(f32)
        value = value * lax.rsqrt(jnp.mean(value * value, axis=-1, keepdims=True) + EPS) * gain
        return value * cos_b + spin(value, LANES // 4) * sin_b

    def turn_a(raw, gain):
        value = raw.astype(f32)
        square = value * value
        first = jnp.sum(jnp.where(low, square, 0.0), axis=-1, keepdims=True)
        second = jnp.sum(jnp.where(low, 0.0, square), axis=-1, keepdims=True)
        mean = jnp.where(low, first, second) * (2.0 / LANES)
        value = value * lax.rsqrt(mean + EPS) * gain
        return value * cos_a + spin(value, LANES // 8) * sin_a

    def twice(ref):
        return jnp.concatenate([ref[...], ref[...]], axis=1)

    raw = jnp.concatenate([ka_t[...].astype(f32), va_t[...].astype(f32)], axis=0).T
    keys = turn_a(raw, twice(gain_ka))
    kv_all[sp, :, 2 * LANES : 3 * LANES] = jnp.where(low, keys, raw).astype(bf16)
    kv_all[sp, :, 0:LANES] = turn_b(k_b[...], gain_kb[...]).astype(bf16)
    kv_all[sp, :, LANES : 2 * LANES] = v_b[...]

    pl.semaphore_wait(barrier, outer + 2)

    def send_kv(source, target, when=None):
        mail.ship(kv_all.at[source], kv_all.at[source], r_kv.at[source], target, when)

    send_kv(sp, above, has_above)
    send_kv(sp, below, has_below)
    send_kv(sp, at_y)

    wide = q_a.shape[1] // LANES
    tall = q_b.shape[1] // LANES
    turned_a = []
    turned_b = []
    for n in range(wide):
        value = turn_a(q_a[:, n * LANES : (n + 1) * LANES], twice(gain_qa))
        other = pltpu.roll(value, LANES // 2, 1)
        for v in (value, other):
            turned_a.append(jnp.where(low, v, 0.0).astype(bf16))
    for n in range(tall):
        value = turn_b(q_b[:, n * LANES : (n + 1) * LANES], gain_qb[...])
        turned_b.append(value.astype(bf16))

    def walk(step, visit):
        for near, far, onward, there in (
            (z >= step, jnp.maximum(z - step, 0), above, has_above),
            (z + step < outer, jnp.minimum(z + step, outer - 1), below, has_below),
        ):
            visit(near, far, onward, jnp.logical_and(near, there))

    def pass_kv(near, far, onward, go):
        source = far * INNER + y

        @pl.when(near)
        def _():
            arrive(kv_all.at[source], r_kv.at[source])

        send_kv(source, onward, go)
        send_kv(source, at_y, near)

    def spread(ends, send):
        for p, target in zip(z_far, at_z):
            edge = jnp.logical_or(p == 0, p == outer - 1)
            send(p, target, edge if ends else jnp.logical_not(edge))

    def send_up(ends):
        def send(p, target, when):
            mail.ship(up_piece(p), up_place(sp), r_up.at[sp], target, when)

        spread(ends, send)

    for step in range(1, outer):
        walk(step, pass_kv)
        if step == max(outer - 2, 1):
            send_up(False)
    mail.ship(up_piece(z), up_place(sp), r_up.at[sp], at_y)

    def forward_up(i):
        source = z_far[i] * INNER + y
        arrive(up_place(source), r_up.at[source])
        mail.ship(up_place(source), up_place(source), r_up.at[source], at_y)

    for k in range(outer):
        source = flip(z, k) * INNER + 1 - y
        arrive(kv_all.at[source], r_kv.at[source])
    send_up(True)
    for h in range(HALVES):
        mail.ship(down_piece(h, z), down_place(h, sp), r_down.at[h, sp], at_y)

    def attend(query, keys, values, scale):
        scores = lax.dot_general(
            query, keys, (((1,), (1,)), ((), ())), preferred_element_type=f32
        )
        scores = scores * scale
        expo = jnp.exp(scores - jnp.max(scores, axis=-1, keepdims=True))
        summed = jnp.dot(expo.astype(bf16), values, preferred_element_type=f32)
        return summed / jnp.sum(expo, axis=-1, keepdims=True)

    both = kv_all[:, :, 2 * LANES : 3 * LANES].reshape(total * count, LANES)
    for n in range(wide):
        first = attend(turned_a[2 * n], both, both, scales[0])
        second = attend(turned_a[2 * n + 1], both, both, scales[0])
        pair = jnp.where(low, pltpu.roll(first, LANES // 2, 1), second)
        attn[:, n * LANES : (n + 1) * LANES] = pair.astype(bf16)
    keys = kv_all[:, :, 0:LANES].reshape(total * count, LANES)
    values = kv_all[:, :, LANES : 2 * LANES].reshape(total * count, LANES)
    for n in range(tall):
        made = attend(turned_b[n], keys, values, scales[1])
        attn[:, (wide + n) * LANES : (wide + n + 1) * LANES] = made.astype(bf16)

    split = wide * LANES
    get_out_a.wait()
    get_out_b.wait()

    def project(p):
        at = pl.ds(pl.multiple_of(p * band, band), band)
        return jnp.dot(attn[at, 0:split], out_a[...], preferred_element_type=f32) + jnp.dot(
            attn[at, split:], out_b[...], preferred_element_type=f32
        )

    for n, side in ((0, 1 - x), (1, x)):
        pc_out[n] = project(side * INNER + 1 - c).astype(bf16)
        mail.ship(pc_out.at[n], pc_in.at[n], r_pc.at[n], at_c)
        if n == 0:
            theirs = project(x_lane)
    arrive(pc_in.at[0], r_pc.at[0])
    px_out[...] = (theirs + pc_in[0].astype(f32)).astype(bf16)
    mail.ship(px_out, px_in, r_px.at[0], at_x)
    get_resid.wait()
    sums = resid[...].astype(f32) + project(tp)
    arrive(pc_in.at[1], r_pc.at[1])
    sums = sums + pc_in[1].astype(f32)
    arrive(px_in, r_px.at[0])
    sums = sums + px_in[...].astype(f32)
    mid[...] = sums.astype(bf16)
    midf = mid[...].astype(f32)
    norm = lax.rsqrt(jnp.mean(midf * midf, axis=-1, keepdims=True) + EPS)
    tokens[z, tp] = (midf * norm * norm_gain[...]).astype(bf16)

    part = band // HALVES

    def some(zz, who, p):
        return tokens.at[zz, who, p * part : (p + 1) * part, :]

    def send_tok(zz, who, p, target, when=None):
        mail.ship(some(zz, who, p), some(zz, who, p), r_tok.at[zz, who, p], target, when)

    for p in range(HALVES):
        send_tok(z, tp, p, above, has_above)
        send_tok(z, tp, p, below, has_below)
        send_tok(z, tp, p, at_x)
    for p in range(HALVES):
        send_tok(z, tp, p, at_c)

    def send_down(ends):
        for h in range(HALVES):

            def send(p, target, when):
                mail.ship(down_piece(h, p), down_place(h, sp), r_down.at[h, sp], target, when)

            spread(ends, send)

    for i in range(outer - 1):
        forward_up(i)

    def relay(near, far, p):
        @pl.when(near)
        def _():
            arrive(some(far, x_lane, p), r_tok.at[far, x_lane, p])

        send_tok(far, x_lane, p, at_c, near)

    always = z >= 0
    for step in range(1, outer):
        for p in range(HALVES):

            def pass_tok(near, far, onward, go):
                @pl.when(near)
                def _():
                    arrive(some(far, tp, p), r_tok.at[far, tp, p])

                send_tok(far, tp, p, onward, go)
                send_tok(far, tp, p, at_x, near)
                send_tok(far, tp, p, at_c, near)

            walk(step, pass_tok)
            if step == 1:
                relay(always, z, p)
            else:
                walk(step - 1, lambda near, far, onward, go: relay(near, far, p))
        if step == 1:
            send_down(False)
        if step == max(outer - 2, 1):
            send_down(True)
    for p in range(HALVES):
        walk(outer - 1, lambda near, far, onward, go: relay(near, far, p))

    def forward_down(h, i):
        source = z_far[i] * INNER + y
        arrive(down_place(h, source), r_down.at[h, source])
        mail.ship(down_place(h, source), down_place(h, source), r_down.at[h, source], at_y)

    get_up.wait()
    for k in range(outer):
        source = flip(z, k) * INNER + 1 - y
        arrive(up_place(source), r_up.at[source])
    for k in range(outer):
        zz = flip(z, k)
        for side in range(SIDES):
            who = side * INNER + 1 - c
            for p in range(HALVES):
                arrive(some(zz, who, p), r_tok.at[zz, who, p])
        block = tokens[zz].reshape(lanes * band, width)
        made = jnp.maximum(jnp.dot(block, up_all[...], preferred_element_type=f32), 0.0)
        hidden[zz] = (made * made).astype(bf16)

    inner = jnp.logical_and(z > 0, z < outer - 1)
    order = list(range(outer - 1, -1, -1))
    mixed = [k for k in order if k not in (outer - 1, 0)] + [outer - 1, 0]
    goals = [jnp.where(inner, flip(z, m), flip(z, k)) for k, m in zip(order, mixed)]

    def compute(h, i):
        n = h * outer + i
        sums = jnp.dot(hidden[goals[i]], down_all[h], preferred_element_type=f32)
        sums = sums.reshape(SIDES, INNER, band, total * slab)
        core_out[n] = jnp.where(c == 0, sums[:, 1], sums[:, 0]).astype(bf16)
        mail.ship(core_out.at[n], core_in.at[n], r_core.at[n], at_c)
        held[i] = jnp.where(c == 0, sums[:, 0], sums[:, 1])

    def exchange(h, i):
        n = h * outer + i
        arrive(core_in.at[n], r_core.at[n])
        mine = held[i] + core_in[n].astype(f32)
        side_out[n] = jnp.where(x == 0, mine[1], mine[0]).astype(bf16)
        mail.ship(side_out.at[n], side_in.at[n], r_side.at[n], at_x)
        total_sum[n] = jnp.where(x == 0, mine[0], mine[1])

    def gather(h, i):
        n = h * outer + i
        arrive(side_in.at[n], r_side.at[n])
        total_sum[n] = total_sum[n] + side_in[n].astype(f32)
        goal = goals[i]
        if i == outer - 1:
            for slot, there in ((z, has_below), (outer, has_above)):

                @pl.when(there)
                def _():
                    arrive(chain_in.at[h, slot], r_chain.at[h, slot])
                    total_sum[n] = total_sum[n] + chain_in[h, slot].astype(f32)

            for j in range(total):
                at = slice((j * HALVES + h) * slab, (j * HALVES + h + 1) * slab)
                value = mid[:, at].astype(f32) + total_sum[n, :, j * slab : (j + 1) * slab]
                out[:, at] = value.astype(out.dtype)
            return
        rising = goal > z
        fed = jnp.where(rising, z > 0, z < outer - 1)

        @pl.when(fed)
        def _():
            arrive(chain_in.at[h, goal], r_chain.at[h, goal])
            total_sum[n] = total_sum[n] + chain_in[h, goal].astype(f32)

        chain_out[n] = total_sum[n].astype(bf16)
        step = jnp.where(rising, z + 1, z - 1)
        slot = jnp.where(jnp.logical_and(step == goal, goal < z), outer, goal)
        target = {"sp": step * INNER + y}
        mail.ship(chain_out.at[n], chain_in.at[h, slot], r_chain.at[h, slot], target)

    def settle(h):
        get_down[h].wait()
        for k in range(outer):
            source = flip(z, k) * INNER + 1 - y
            arrive(down_place(h, source), r_down.at[h, source])

    def start_half(h):
        settle(h)
        for i in range(outer):
            compute(h, i)
        for i in range(outer):
            exchange(h, i)

    for i in range(outer - 1):
        forward_down(0, i)
    start_half(0)
    for i in range(outer - 1):
        forward_down(1, i)
    for i in range(2):
        gather(0, i)
    start_half(1)
    for i in range(2, outer):
        gather(0, i)
    for i in range(outer):
        gather(1, i)
    mail.close()


def layer(operands, total, lanes):
    q_a, q_b, resid = operands[4], operands[5], operands[13]
    up, down = operands[16], operands[17]
    count = q_a.shape[0]
    outer = total // INNER
    band, width = resid.shape
    units = up.shape[1] // outer
    kind = jnp.bfloat16
    scales = ((LANES // 2) ** (-0.5), LANES ** (-0.5))
    features = q_a.shape[1] + q_b.shape[1]
    vmem = pl.BlockSpec(memory_space=pltpu.VMEM)
    hbm = pl.BlockSpec(memory_space=pltpu.HBM)
    sems = pltpu.SemaphoreType.DMA
    slab = down.shape[1] // HALVES
    broad = slab * total
    items = outer * HALVES
    scratch = [
        pltpu.VMEM(resid.shape, kind),
        pltpu.VMEM(operands[14].shape, kind),
        pltpu.VMEM(operands[15].shape, kind),
        pltpu.VMEM((total, count, 3 * LANES), kind),
        pltpu.VMEM((count, features), kind),
        pltpu.VMEM((up.shape[0] * total, units), kind),
        pltpu.VMEM((HALVES, units, broad), kind),
        pltpu.VMEM((2, band, width), kind),
        pltpu.VMEM((2, band, width), kind),
        pltpu.VMEM((band, width), kind),
        pltpu.VMEM((band, width), kind),
        pltpu.VMEM((band, width), kind),
        pltpu.VMEM((outer, lanes, band, width), kind),
        pltpu.VMEM((outer, lanes * band, units), kind),
        pltpu.VMEM((items, SIDES, band, broad), kind),
        pltpu.VMEM((items, SIDES, band, broad), kind),
        pltpu.VMEM((items, band, broad), kind),
        pltpu.VMEM((items, band, broad), kind),
        pltpu.VMEM((items, band, broad), kind),
        pltpu.VMEM((HALVES, outer + 1, band, broad), kind),
        pltpu.VMEM((outer, SIDES, band, broad), jnp.float32),
        pltpu.VMEM((items, band, broad), jnp.float32),
        sems((200,)),
        sems((8,)),
        sems((total,)),
        sems((total,)),
        sems((HALVES, total)),
        sems((2,)),
        sems((1,)),
        sems((outer, lanes, HALVES)),
        sems((items,)),
        sems((items,)),
        sems((HALVES, outer + 1)),
    ]
    return pl.pallas_call(
        lambda *refs: layer_kernel(outer, scales, *refs),
        out_shape=jax.ShapeDtypeStruct(resid.shape, resid.dtype),
        in_specs=[vmem] * 13 + [hbm] * 5,
        out_specs=vmem,
        scratch_shapes=scratch,
        compiler_params=pltpu.CompilerParams(
            collective_id=0, has_side_effects=True, vmem_limit_bytes=60 * 1024 * 1024
        ),
        name="layer",
    )(*operands)


def turning_tables(steps, widths, first):
    spots = np.arange(steps, dtype=np.float32)[:, None]
    pieces = []
    for width in widths:
        index = np.arange(LANES) % width
        freqs = (10000.0 ** (-(2.0 * (index % (width // 4))) / (width // 2))).astype(np.float32)
        angles = (spots * freqs).astype(np.float64)
        mine = (index < width // 2) == first
        pieces += [np.where(mine, np.cos(angles), 0.0), np.where(mine, np.sin(angles), 0.0)]
    return jnp.asarray(np.concatenate(pieces, axis=1), jnp.float32)


def kernel_local(
    total,
    lanes,
    resid,
    query_a,
    key_a,
    value_a,
    query_b,
    key_b,
    value_b,
    gain_qa,
    gain_ka,
    gain_qb,
    gain_kb,
    w_out_a,
    w_out_b,
    norm_gain,
    w_up,
    w_down,
):
    widths = (gain_qa.shape[0], gain_qb.shape[0])
    row_table = turning_tables(query_a.shape[0] * total // GRID_W, widths, True)
    col_table = turning_tables(GRID_W, widths, False)
    gains = [g.reshape(1, -1) for g in (gain_qa, gain_ka, gain_qb, gain_kb, norm_gain)]
    operands = [key_a.T, value_a.T, key_b, value_b, query_a, query_b, row_table, col_table]
    operands += gains + [resid, w_out_a, w_out_b, w_up, w_down]
    return layer(operands, total, lanes)


def fits(total, lanes, args):
    outer = total // INNER
    if total % INNER or lanes != INNER * SIDES or outer < 2 or outer & (outer - 1):
        return False
    key_a, key_b, gain_a, gain_b = args[2], args[5], args[7], args[9]
    if 2 * gain_a.shape[0] != LANES or gain_b.shape[0] != LANES:
        return False
    if key_a.shape[1] != lanes * LANES // 2 or key_b.shape[1] != lanes * LANES:
        return False
    if args[1].shape[1] % (lanes * LANES) or args[4].shape[1] % (lanes * LANES):
        return False
    if args[1].shape[0] % (total * GRID_W) or args[0].shape[0] % (total * lanes * HALVES * 16):
        return False
    w_up, w_down = args[-2], args[-1]
    units = w_up.shape[1] // lanes // outer
    rows = w_up.shape[0] // total
    cols = w_down.shape[1] // total
    small = units * w_up.shape[0] <= 2**20 and args[0].shape[0] <= 2**11
    return units % LANES == 0 and rows % 16 == 0 and cols % (HALVES * LANES) == 0 and small


def sharded(inside, mesh):
    return jax.shard_map(
        inside,
        mesh=mesh,
        in_specs=(
            P(("sp", "tp"), None),
            P("sp", "tp"),
            P("sp", "tp"),
            P("sp", "tp"),
            P("sp", "tp"),
            P("sp", "tp"),
            P("sp", "tp"),
            P(),
            P(),
            P(),
            P(),
            P("tp", None),
            P("tp", None),
            P(),
            P("sp", "tp"),
            P("tp", "sp"),
        ),
        out_specs=P(("sp", "tp"), None),
        check_vma=False,
    )


def solution(mesh):
    total = mesh.shape["sp"]
    lanes = mesh.shape["tp"]

    def run(*args):
        inside = local
        if fits(total, lanes, args):
            inside = lambda *shards: kernel_local(total, lanes, *shards)
        return sharded(inside, mesh)(*args)

    return run
```
